32 devices in a mesh: sp: 8 (over z, y), tp: 4 (over x, core).
Axes of the slice: x: 2, y: 2, z: 4, core: 2. Of those that a mesh axis runs over, the one named last changes fastest.
Arguments:
- hidden: bfloat16 [1024, 2048], P('sp'), may hold values from -6 to 6
- value_weight: bfloat16 [2048, 4096], P(None, 'tp'), may hold values from -0.125 to 0.125
- key_vecs: bfloat16 [1024, 8, 128], P('sp', 'tp'), may hold values from -0.29882812 to 0.29882812
- queries: bfloat16 [1024, 8, 128], P('sp', 'tp'), may hold values from -0.29882812 to 0.29882812
- decay_pre: float32 [1024, 64], P('sp', 'tp'), may hold values from -4 to 4
- decay_rate: float32 [64], P('tp'), may hold values from 5.859375e-05 to 0.0036132813
- cotangent: bfloat16 [1024, 64, 64], P('sp', 'tp'), may hold values from -1.1953125 to 1.1953125
Outputs:
- grad_keys: bfloat16 [1024, 8, 128], P('sp', 'tp')
- grad_queries: bfloat16 [1024, 8, 128], P('sp', 'tp')
- grad_decay: float32 [1024, 64], P('sp', 'tp')
- grad_hidden: bfloat16 [1024, 2048], P(('sp', 'tp'))
- grad_weight: float32 [2048, 4096], P('sp', 'tp')
The draws below stay inside these ranges and needn't reach their ends.
All inputs are finite; a program needn't handle non-finite values.
Results may differ from the reference program's by a relative error of at most 0.003.
Values sent between devices are 32-bit elements.
A program may use at most 64 MiB of HBM per device.

```python
import math
import jax
import jax.numpy as jnp
from jax import lax

D = 2048
HEADS = 64
HEAD_DIM = 64
GROUPS = 8
STATE = 128
TOK_DEV = 128
INNER = 4096
TOKENS = 1024


def shard_levels(rng, shape, pieces, smallest, top_value):
    level = 1.0
    for axis_at, shards_of in pieces:
        heights = jax.random.uniform(jax.random.fold_in(jax.random.fold_in(rng, 6), axis_at), (shards_of,), jnp.float32, smallest / len(pieces), top_value / len(pieces))
        level = level * jnp.repeat(jnp.exp(heights), shape[axis_at] // shards_of).reshape((-1,) + (1,) * (len(shape) - 1 - axis_at))
    return level


def bell_draw(rng, dims, scale, limit, shards=(), kind=jnp.bfloat16):
    entries = scale * jax.random.normal(rng, dims, jnp.float32)
    if shards:
        entries = entries * shard_levels(rng, dims, shards, -0.22, 0.18)
    return jnp.clip(entries, -limit, limit).astype(kind)


def setup_inputs(seed: int = 0) -> dict:
    splits = jax.random.split(jax.random.key(seed), 8)
    return {
        "hidden": bell_draw(splits[0], (TOKENS, D), 1.0, 6.0, ((0, 8),)),
        "value_weight": bell_draw(splits[1], (D, INNER), D ** -0.5, 0.125, ((1, 4),)),
        "key_vecs": bell_draw(splits[2], (TOKENS, GROUPS, STATE), 0.05, 0.29882812, ((0, 8), (1, 4))),
        "queries": bell_draw(splits[3], (TOKENS, GROUPS, STATE), 0.05, 0.29882812, ((0, 8), (1, 4))),
        "decay_pre": bell_draw(splits[4], (TOKENS, HEADS), 1.0, 4.0, ((0, 8), (1, 4)), jnp.float32),
        "decay_rate": jnp.clip(jnp.exp(math.log(0.0036132813) - 4.1217436 * jax.random.uniform(splits[5], (HEADS,), jnp.float32) ** shard_levels(splits[5], (HEADS,), ((0, 4),), -0.2, 0.2)), 5.859374869032763e-05, 0.0036132813),
        "cotangent": bell_draw(splits[6], (TOKENS, HEADS, HEAD_DIM), 0.2, 1.1953125, ((0, 8), (1, 4))),
    }


highest = lax.Precision.HIGHEST

def local_mixer(values_f, keys_f, queries_f, decay_pre, decay_rate, state_in):
    heads_here = values_f.shape[1]
    per_group = heads_here // keys_f.shape[1]
    key_heads = jnp.repeat(keys_f, per_group, axis=1)
    query_heads = jnp.repeat(queries_f, per_group, axis=1)
    log_decay = -decay_rate[None, :] * jax.nn.softplus(decay_pre)
    cumulative = jnp.cumsum(log_decay, axis=0)
    length = values_f.shape[0]
    causal = jnp.tril(jnp.ones((length, length), dtype=bool))[None]
    across = cumulative.T[:, :, None] - cumulative.T[:, None, :]
    damping = jnp.where(causal, jnp.exp(jnp.where(causal, across, 0.0)), 0.0)
    scores = jnp.einsum('thn,shn->hts', query_heads, key_heads, precision=highest)
    outputs = jnp.einsum('hts,shp->thp', scores * damping, values_f, precision=highest)
    carried = jnp.einsum('thn,hpn->thp', query_heads, state_in, precision=highest)
    outputs = outputs + jnp.exp(cumulative)[:, :, None] * carried
    to_end = jnp.exp(cumulative[-1][None, :] - cumulative)
    state_out = jnp.exp(cumulative[-1])[:, None, None] * state_in + jnp.einsum('sh,shp,shn->hpn', to_end, values_f, key_heads, precision=highest)
    return (outputs, state_out)

def reference(hidden, value_weight, key_vecs, queries, decay_pre, decay_rate, cotangent):
    values = jnp.dot(hidden, value_weight, preferred_element_type=jnp.float32).astype(jnp.bfloat16)
    tokens_all = hidden.shape[0]
    block_count = tokens_all // TOK_DEV
    head_count = decay_rate.shape[0]

    def to_blocks(tensor):
        return tensor.reshape((block_count, TOK_DEV) + tensor.shape[1:])

    def whole_seq(values_in, keys_in, queries_in, pre_in):

        def advance(state_now, inputs):
            block_out, state_next = local_mixer(inputs[0], inputs[1], inputs[2], inputs[3], decay_rate, state_now)
            return (state_next, block_out)
        start_state = jnp.zeros((head_count, HEAD_DIM, STATE), jnp.float32)
        final_state, block_outs = lax.scan(advance, start_state, (to_blocks(values_in), to_blocks(keys_in), to_blocks(queries_in), to_blocks(pre_in)))
        return block_outs.reshape((tokens_all,) + block_outs.shape[2:])
    values_f = values.reshape(tokens_all, head_count, HEAD_DIM).astype(jnp.float32)
    primal, pullback = jax.vjp(whole_seq, values_f, key_vecs.astype(jnp.float32), queries.astype(jnp.float32), decay_pre)
    grad_values, grad_keys, grad_queries, grad_decay = pullback(cotangent.astype(jnp.float32))
    grad_flat = grad_values.reshape(tokens_all, -1).astype(jnp.bfloat16)
    grad_hidden = lax.dot_general(grad_flat, value_weight, (((1,), (1,)), ((), ())), preferred_element_type=jnp.float32).astype(jnp.bfloat16)
    grad_weight = lax.dot_general(hidden, grad_flat, (((0,), (0,)), ((), ())), preferred_element_type=jnp.float32)
    return (grad_keys.astype(jnp.bfloat16), grad_queries.astype(jnp.bfloat16), grad_decay, grad_hidden, grad_weight)
```

```python
import functools

import jax
import jax.numpy as jnp
from jax import lax
from jax.experimental import pallas as pl
from jax.experimental.pallas import tpu as pltpu
from jax.sharding import PartitionSpec as P

MESH = pl.DeviceIdType.MESH
F32 = jnp.float32
BF16 = jnp.bfloat16


def inner_size(count):
    size = 1
    while size * size * 4 <= count:
        size *= 2
    while count % size:
        size -= 1
    return size


def remote(src, dst, send, recv, axis, index):
    return pltpu.make_async_remote_copy(
        src_ref=src, dst_ref=dst, send_sem=send, recv_sem=recv, device_id={axis: index}, device_id_type=MESH
    )


def scan_kernel(ny, nz, both_ref, dec_ref, hid_ref, out_ref, hcol_ref,
                ybuf, ydec, pin, pout, hid_f, hland,
                ysend, yrecv, dsend, drecv, psend, precv, hsend, hrecv):
    me = lax.axis_index("sp")
    z, y = me // ny, me % ny
    heads = both_ref.shape[0]
    span = hland.shape[2]

    barrier = pltpu.get_barrier_semaphore()
    for dy in range(1, ny):
        pl.semaphore_signal(barrier, inc=1, device_id={"sp": z * ny + (y + dy) % ny}, device_id_type=MESH)
    for dz in range(1, nz):
        pl.semaphore_signal(barrier, inc=1, device_id={"sp": ((z + dz) % nz) * ny + y}, device_id_type=MESH)
    pl.semaphore_wait(barrier, ny - 1 + nz - 1)

    def ycopy(h, dy):
        there = (y + dy) % ny
        return remote(both_ref.at[h], ybuf.at[y, h], ysend.at[there, h], yrecv.at[y, h], "sp", z * ny + there)

    def yarrive(h, there):
        return remote(both_ref.at[h], ybuf.at[there, h], ysend.at[there, h], yrecv.at[there, h], "sp", z * ny + there)

    def dcopy(dy):
        there = (y + dy) % ny
        return remote(dec_ref, ydec.at[y], dsend.at[there], drecv.at[y], "sp", z * ny + there)

    def darrive(dy):
        there = (y + dy) % ny
        return remote(dec_ref, ydec.at[there], dsend.at[there], drecv.at[there], "sp", z * ny + there)

    for dy in range(1, ny):
        dcopy(dy).start()

    def launch(h, carry):
        for dy in range(1, ny):
            ycopy(h, dy).start()
        return carry

    lax.fori_loop(0, heads, launch, 0)

    def hcopy(dz):
        there = (z + dz) % nz
        return remote(
            hid_f.at[:, pl.ds(pl.multiple_of(there * span, 128), span)], hland.at[z],
            hsend.at[there], hrecv.at[z], "sp", there * ny + y,
        )

    def harrive(dz):
        there = (z + dz) % nz
        return remote(
            hid_f.at[:, pl.ds(pl.multiple_of(there * span, 128), span)], hland.at[there],
            hsend.at[there], hrecv.at[there], "sp", there * ny + y,
        )

    hid_f[...] = hid_ref[...].astype(F32)
    for dz in range(1, nz):
        hcopy(dz).start()
    ybuf[y] = both_ref[...]
    ydec[y] = dec_ref[...]
    for dy in range(1, ny):
        darrive(dy).wait_recv()

    @pl.when(z == 0)
    def _():
        pin[0] = jnp.zeros_like(pin[0])

    @pl.when(z == nz - 1)
    def _():
        pin[1] = jnp.zeros_like(pin[1])

    def up(h):
        return remote(pout.at[0, h], pin.at[0, h], psend.at[0, h], precv.at[0, h], "sp", me + ny)

    def down(h):
        return remote(pout.at[1, h], pin.at[1, h], psend.at[1, h], precv.at[1, h], "sp", me - ny)

    def ready(h, first):
        @pl.when(first)
        def _():
            for dy in range(1, ny):
                yarrive(h, (y + dy) % ny).wait_recv()

    def step(t, carry):
        a = t - z
        b = t - (nz - 1 - z)

        @pl.when((a >= 0) & (a < heads))
        def _():
            ready(a, (2 * z <= nz - 1))

            @pl.when(z > 0)
            def _():
                up(a).wait_recv()

            now = pin[0, a]
            for yy in range(ny):
                @pl.when(y == yy)
                def _():
                    out_ref[a, 0] = now

                now = ydec[yy, a] * now + ybuf[yy, a, 0]
            pout[0, a] = now

            @pl.when(z < nz - 1)
            def _():
                up(a).start()

        @pl.when((b >= 0) & (b < heads))
        def _():
            ready(b, (2 * z > nz - 1))

            @pl.when(z < nz - 1)
            def _():
                down(b).wait_recv()

            now = pin[1, b]
            for yy in reversed(range(ny)):
                @pl.when(y == yy)
                def _():
                    out_ref[b, 1] = now

                now = ydec[yy, b] * now + ybuf[yy, b, 1]
            pout[1, b] = now

            @pl.when(z > 0)
            def _():
                down(b).start()

        return carry

    lax.fori_loop(0, heads + nz - 1, step, 0)

    hcol_ref[pl.ds(pl.multiple_of(z * hland.shape[1], 128), hland.shape[1]), :] = (
        hid_f[:, pl.ds(pl.multiple_of(z * span, 128), span)].astype(BF16)
    )
    for dz in range(1, nz):
        there = (z + dz) % nz
        harrive(dz).wait_recv()
        hcol_ref[pl.ds(pl.multiple_of(there * hland.shape[1], 128), hland.shape[1]), :] = hland[there].astype(BF16)
    for dz in range(1, nz):
        hcopy(dz).wait_send()
    for dy in range(1, ny):
        dcopy(dy).wait_send()

    def drain(h, carry):
        for dy in range(1, ny):
            ycopy(h, dy).wait_send()

        @pl.when(z < nz - 1)
        def _():
            up(h).wait_send()

        @pl.when(z > 0)
        def _():
            down(h).wait_send()

        return carry

    lax.fori_loop(0, heads, drain, 0)


def grads_kernel(ny, nz, ntp, width, gv_ref, hct_ref, ghp_ref, gw_ref, gh_ref,
                 gath, part, land, ghland,
                 upsend, dnsend, grecv, ysend, yrecv, hsend, hrecv):
    me = lax.axis_index("sp")
    mine = lax.axis_index("tp")
    z, y = me // ny, me % ny
    rows = gw_ref.shape[0]
    chunks = gv_ref.shape[1] // width
    length = gv_ref.shape[0]
    own_rows = gh_ref.shape[0]

    barrier = pltpu.get_barrier_semaphore()
    for dy in range(1, ny):
        pl.semaphore_signal(barrier, inc=1, device_id={"sp": z * ny + (y + dy) % ny}, device_id_type=MESH)
    for dz in (1, nz - 1):
        pl.semaphore_signal(barrier, inc=1, device_id={"sp": ((z + dz) % nz) * ny + y}, device_id_type=MESH)
    for dt in range(1, ntp):
        pl.semaphore_signal(barrier, inc=1, device_id={"tp": (mine + dt) % ntp}, device_id_type=MESH)
    pl.semaphore_wait(barrier, ny - 1 + 2 + ntp - 1)

    def cols(c):
        return pl.ds(pl.multiple_of(c * width, 128), width)

    def up(b, c):
        return remote(gath.at[b, c], gath.at[b, c], upsend.at[b, c], grecv.at[b, c], "sp", me + ny)

    def down(b, c):
        return remote(gath.at[b, c], gath.at[b, c], dnsend.at[b, c], grecv.at[b, c], "sp", me - ny)

    def launch(c, carry):
        gath[z, c] = gv_ref[:, cols(c)]

        @pl.when(z < nz - 1)
        def _():
            up(z, c).start()

        @pl.when(z > 0)
        def _():
            down(z, c).start()

        return carry

    lax.fori_loop(0, chunks, launch, 0)

    def hcopy(dt):
        there = (mine + dt) % ntp
        return remote(
            ghp_ref.at[pl.ds(pl.multiple_of(there * own_rows, 8), own_rows), :], ghland.at[mine],
            hsend.at[there], hrecv.at[mine], "tp", there,
        )

    def harrive(dt):
        there = (mine + dt) % ntp
        return remote(
            ghp_ref.at[pl.ds(pl.multiple_of(there * own_rows, 8), own_rows), :], ghland.at[there],
            hsend.at[there], hrecv.at[there], "tp", there,
        )

    for dt in range(1, ntp):
        hcopy(dt).start()

    def ycopy(c, there):
        return remote(
            part.at[there, c], land.at[y, c], ysend.at[there, c], yrecv.at[y, c], "sp", z * ny + there
        )

    def yarrive(c, there):
        return remote(
            part.at[there, c], land.at[there, c], ysend.at[there, c], yrecv.at[there, c], "sp", z * ny + there
        )

    def work(c, carry):
        for d in range(1, nz):
            low, high = z - d, z + d

            @pl.when(low >= 0)
            def _():
                down(jnp.maximum(low, 0), c).wait_recv()

                @pl.when(z < nz - 1)
                def _():
                    up(jnp.maximum(low, 0), c).start()

            @pl.when(high < nz)
            def _():
                up(jnp.minimum(high, nz - 1), c).wait_recv()

                @pl.when(z > 0)
                def _():
                    down(jnp.minimum(high, nz - 1), c).start()

        block = gath[:, c].reshape(nz * length, width).astype(BF16)
        for dy in range(1, ny):
            there = (y + dy) % ny
            part[there, c] = jnp.dot(
                hct_ref[pl.ds(pl.multiple_of(there * rows, 8), rows), :], block, preferred_element_type=F32
            )
            ycopy(c, there).start()
        gw_ref[:, cols(c)] = jnp.dot(
            hct_ref[pl.ds(pl.multiple_of(y * rows, 8), rows), :], block, preferred_element_type=F32
        )
        return carry

    lax.fori_loop(0, chunks, work, 0)

    total = ghp_ref[pl.ds(pl.multiple_of(mine * own_rows, 8), own_rows), :]
    for dt in range(1, ntp):
        harrive(dt).wait_recv()
        total = total + ghland[(mine + dt) % ntp]
    gh_ref[...] = total.astype(gh_ref.dtype)

    def collect(c, carry):
        for dy in range(1, ny):
            there = (y + dy) % ny
            yarrive(c, there).wait_recv()
            gw_ref[:, cols(c)] += land[there, c]
        return carry

    lax.fori_loop(0, chunks, collect, 0)

    def drain(c, carry):
        for dy in range(1, ny):
            ycopy(c, (y + dy) % ny).wait_send()
        for b in range(nz):
            @pl.when((b <= z) & (z < nz - 1))
            def _():
                up(b, c).wait_send()

            @pl.when((b >= z) & (z > 0))
            def _():
                down(b, c).wait_send()

        return carry

    lax.fori_loop(0, chunks, drain, 0)
    for dt in range(1, ntp):
        hcopy(dt).wait_send()


VM = pl.BlockSpec(memory_space=pltpu.VMEM)
LIMIT = 48 * 1024 * 1024


def split(x):
    hi = lax.reduce_precision(x, 8, 7)
    return hi.astype(BF16), (x - hi).astype(BF16)


def two_pass(spec, x, y):
    hi, lo = split(x)
    return jnp.einsum(spec, hi, y, preferred_element_type=F32) + jnp.einsum(spec, lo, y, preferred_element_type=F32)


def per_device(sp, tp, hidden, value_weight, key_vecs, queries, decay_pre, decay_rate, cotangent):
    length = hidden.shape[0]
    heads = decay_rate.shape[0]
    head_width = cotangent.shape[2]
    groups = key_vecs.shape[1]
    state = key_vecs.shape[2]
    per = heads // groups
    features = hidden.shape[1]
    columns = value_weight.shape[1]
    ny = inner_size(sp)
    nz = sp // ny
    values = jnp.dot(hidden, value_weight, preferred_element_type=F32).astype(BF16)
    v = values.reshape(length, groups, per, head_width)
    cot = cotangent.reshape(length, groups, per, head_width)
    log_decay = -decay_rate[None, :] * jax.nn.softplus(decay_pre)
    tri = jnp.tril(jnp.ones((length, length), F32))
    cum = jnp.dot(tri, log_decay, precision=lax.Precision.HIGHEST)
    tot = cum[-1]
    to_end = jnp.exp(tot[None] - cum).reshape(length, groups, per, 1)
    ecum = jnp.exp(cum).reshape(length, groups, per, 1)
    local_state = two_pass("sgip,sgn->gipn", to_end * v.astype(F32), key_vecs)
    local_pull = two_pass("sgip,sgn->gipn", ecum * cot.astype(F32), queries)
    both = jnp.stack([local_state, local_pull], axis=2).reshape(heads, 2, head_width, state)
    dec = jnp.broadcast_to(jnp.exp(tot)[:, None, None], (heads, 1, state))
    span = features // nz
    scanned, hcol = pl.pallas_call(
        functools.partial(scan_kernel, ny, nz),
        out_shape=(
            jax.ShapeDtypeStruct(both.shape, F32),
            jax.ShapeDtypeStruct((nz * length, span), BF16),
        ),
        in_specs=[VM] * 3,
        out_specs=(VM, VM),
        scratch_shapes=[
            pltpu.VMEM((ny,) + both.shape, F32),
            pltpu.VMEM((ny,) + dec.shape, F32),
            pltpu.VMEM((2, heads, head_width, state), F32),
            pltpu.VMEM((2, heads, head_width, state), F32),
            pltpu.VMEM((length, features), F32),
            pltpu.VMEM((nz, length, span), F32),
            pltpu.SemaphoreType.DMA((ny, heads)),
            pltpu.SemaphoreType.DMA((ny, heads)),
            pltpu.SemaphoreType.DMA((ny,)),
            pltpu.SemaphoreType.DMA((ny,)),
            pltpu.SemaphoreType.DMA((2, heads)),
            pltpu.SemaphoreType.DMA((2, heads)),
            pltpu.SemaphoreType.DMA((nz,)),
            pltpu.SemaphoreType.DMA((nz,)),
        ],
        compiler_params=pltpu.CompilerParams(collective_id=0, has_side_effects=True, vmem_limit_bytes=LIMIT),
        name="scan_states",
    )(both, dec, hidden)
    state_in = scanned[:, 0].reshape(groups, per, head_width, state)
    state_grad = scanned[:, 1].reshape(groups, per, head_width, state)

    cum_h = cum.T
    causal = jnp.tril(jnp.ones((length, length), dtype=bool))[None]
    across = cum_h[:, :, None] - cum_h[:, None, :]
    damping = jnp.where(causal, jnp.exp(jnp.where(causal, across, 0.0)), 0.0).reshape(groups, per, length, length)
    scores = jnp.einsum("tgn,sgn->gts", queries, key_vecs, preferred_element_type=F32)
    pair = jnp.einsum("tgip,sgip->gits", cot, v, preferred_element_type=F32)
    dscore = pair * damping
    flux = dscore * scores[:, None]
    net = (jnp.sum(flux, axis=3) - jnp.sum(flux, axis=2)).reshape(heads, length).T
    dsum = jnp.sum(dscore, axis=1)
    mixed = (scores[:, None] * damping).astype(BF16)
    gq_heads = ecum * two_pass("gipn,tgip->tgin", state_in, cot)
    gk_heads = to_end * two_pass("gipn,tgip->tgin", state_grad, v)
    gv = jnp.einsum("gits,tgip->sgip", mixed, cot, preferred_element_type=F32) + to_end * two_pass(
        "gipn,sgn->sgip", state_grad, key_vecs
    )
    gq = two_pass("gts,sgn->tgn", dsum, key_vecs) + jnp.sum(gq_heads, axis=2)
    gk = two_pass("gts,tgn->sgn", dsum, queries) + jnp.sum(gk_heads, axis=2)
    qgq = jnp.sum(gq_heads * queries.astype(F32)[:, :, None], axis=3).reshape(length, heads)
    kgk = jnp.sum(gk_heads * key_vecs.astype(F32)[:, :, None], axis=3).reshape(length, heads)
    through = jnp.exp(tot) * jnp.sum(state_in * state_grad, axis=(2, 3)).reshape(heads)
    suffix = jnp.dot(tri.T, net + qgq, precision=lax.Precision.HIGHEST)
    prefix = jnp.dot(tri - jnp.eye(length, dtype=F32), kgk, precision=lax.Precision.HIGHEST)
    grad_decay = (suffix + prefix + through[None]) * -decay_rate[None] * jax.nn.sigmoid(decay_pre)

    grad_flat = gv.reshape(length, columns).astype(BF16)
    ghp = lax.dot_general(grad_flat, value_weight, (((1,), (1,)), ((), ())), preferred_element_type=F32)
    rows = features // sp
    width = min(columns, 128)
    chunks = columns // width
    grad_weight, grad_hidden = pl.pallas_call(
        functools.partial(grads_kernel, ny, nz, tp, width),
        out_shape=(
            jax.ShapeDtypeStruct((rows, columns), F32),
            jax.ShapeDtypeStruct((length // tp, features), BF16),
        ),
        in_specs=[VM] * 3,
        out_specs=(VM, VM),
        scratch_shapes=[
            pltpu.VMEM((nz, chunks, length, width), F32),
            pltpu.VMEM((ny, chunks, rows, width), F32),
            pltpu.VMEM((ny, chunks, rows, width), F32),
            pltpu.VMEM((tp, length // tp, features), F32),
            pltpu.SemaphoreType.DMA((nz, chunks)),
            pltpu.SemaphoreType.DMA((nz, chunks)),
            pltpu.SemaphoreType.DMA((nz, chunks)),
            pltpu.SemaphoreType.DMA((ny, chunks)),
            pltpu.SemaphoreType.DMA((ny, chunks)),
            pltpu.SemaphoreType.DMA((tp,)),
            pltpu.SemaphoreType.DMA((tp,)),
        ],
        compiler_params=pltpu.CompilerParams(collective_id=1, has_side_effects=True, vmem_limit_bytes=LIMIT),
        name="weight_grads",
    )(grad_flat.astype(F32), hcol.T, ghp)
    return (gq_cast(gk), gq_cast(gq), grad_decay, grad_hidden, grad_weight)


def gq_cast(x):
    return x.astype(BF16)


def solution(mesh):
    return jax.shard_map(
        functools.partial(per_device, mesh.shape["sp"], mesh.shape["tp"]),
        mesh=mesh,
        in_specs=(
            P("sp", None),
            P(None, "tp"),
            P("sp", "tp", None),
            P("sp", "tp", None),
            P("sp", "tp"),
            P("tp"),
            P("sp", "tp", None),
        ),
        out_specs=(
            P("sp", "tp", None),
            P("sp", "tp", None),
            P("sp", "tp"),
            P(("sp", "tp"), None),
            P("sp", "tp"),
        ),
        check_vma=False,
    )
```

```python
import functools

import jax
import jax.numpy as jnp
from jax import lax
from jax.experimental import pallas as pl
from jax.experimental.pallas import tpu as pltpu
from jax.sharding import PartitionSpec as P

MESH = pl.DeviceIdType.MESH
F32 = jnp.float32
BF16 = jnp.bfloat16


def inner_size(count):
    size = 1
    while size * size * 4 <= count:
        size *= 2
    while count % size:
        size -= 1
    return size


def remote(src, dst, send, recv, axis, index):
    return pltpu.make_async_remote_copy(
        src_ref=src, dst_ref=dst, send_sem=send, recv_sem=recv, device_id={axis: index}, device_id_type=MESH
    )


def scan_kernel(ny, nz, ntp, skew, pieces, both_ref, dec_ref, hid_ref, out_ref, hcol_ref,
                ybuf, ydec, pin, pout, hid_f, hland,
                ysend, yrecv, dsend, drecv, psend, precv, hsend, hrecv, fsend, frecv):
    me = lax.axis_index("sp")
    z, y = me // ny, me % ny
    heads = both_ref.shape[0]
    span = hland.shape[2]

    barrier = pltpu.get_barrier_semaphore()
    for dy in range(1, ny):
        pl.semaphore_signal(barrier, inc=1, device_id={"sp": z * ny + (y + dy) % ny}, device_id_type=MESH)
    for dz in range(1, nz):
        pl.semaphore_signal(barrier, inc=1, device_id={"sp": ((z + dz) % nz) * ny + y}, device_id_type=MESH)
    mine = lax.axis_index("tp")
    halves = 2 if ntp % 2 == 0 else 1
    half = mine % halves
    other = mine + 1 - 2 * half
    if halves == 2:
        pl.semaphore_signal(barrier, inc=1, device_id={"tp": other}, device_id_type=MESH)
    pl.semaphore_wait(barrier, ny - 1 + nz - 1 + halves - 1)
    half_rows = hland.shape[1] // halves
    piece_rows = half_rows // pieces

    def ycopy(h, dy):
        there = (y + dy) % ny
        return remote(both_ref.at[h], ybuf.at[y, h], ysend.at[there, h], yrecv.at[y, h], "sp", z * ny + there)

    def yarrive(h, there):
        return remote(both_ref.at[h], ybuf.at[there, h], ysend.at[there, h], yrecv.at[there, h], "sp", z * ny + there)

    def dcopy(dy):
        there = (y + dy) % ny
        return remote(dec_ref, ydec.at[y], dsend.at[there], drecv.at[y], "sp", z * ny + there)

    def darrive(dy):
        there = (y + dy) % ny
        return remote(dec_ref, ydec.at[there], dsend.at[there], drecv.at[there], "sp", z * ny + there)

    for dy in range(1, ny):
        dcopy(dy).start()

    def launch(h, carry):
        for dy in range(1, ny):
            ycopy(h, dy).start()
        return carry

    lax.fori_loop(0, heads, launch, 0)

    def piece(p):
        return pl.ds(pl.multiple_of(half * half_rows + p * piece_rows, 8), piece_rows)

    def columns_of(plane):
        return pl.ds(pl.multiple_of(plane * span, 128), span)

    def hcopy(dz, p):
        there = (z + dz) % nz
        return remote(
            hid_f.at[piece(p), columns_of(there)], hland.at[z, piece(p)],
            hsend.at[there, p], hrecv.at[z, p], "sp", there * ny + y,
        )

    def harrive(dz, p):
        there = (z + dz) % nz
        return remote(
            hid_f.at[piece(p), columns_of(there)], hland.at[there, piece(p)],
            hsend.at[there, p], hrecv.at[there, p], "sp", there * ny + y,
        )

    def share(dz, part):
        there = (z + dz) % nz
        block = hland.at[there, pl.ds(pl.multiple_of(part * half_rows, 8), half_rows)]
        return remote(block, block, fsend.at[there], frecv.at[there], "tp", other)

    hid_f[...] = hid_ref[...].astype(F32)
    ybuf[y] = both_ref[...]
    ydec[y] = dec_ref[...]
    for dy in range(1, ny):
        darrive(dy).wait_recv()

    @pl.when(z == 0)
    def _():
        pin[0] = jnp.zeros_like(pin[0])

    @pl.when(z == nz - 1)
    def _():
        pin[1] = jnp.zeros_like(pin[1])

    def up(h):
        return remote(pout.at[0, h], pin.at[0, h], psend.at[0, h], precv.at[0, h], "sp", me + ny)

    def down(h):
        return remote(pout.at[1, h], pin.at[1, h], psend.at[1, h], precv.at[1, h], "sp", me - ny)

    def ready(h, first):
        @pl.when(first)
        def _():
            for dy in range(1, ny):
                yarrive(h, (y + dy) % ny).wait_recv()

    def step(t, carry):
        a = t - skew * z
        b = t - skew * (nz - 1 - z)

        @pl.when((a >= 0) & (a < heads))
        def _():
            ready(a, (2 * z <= nz - 1))

            @pl.when(z > 0)
            def _():
                up(a).wait_recv()

            now = pin[0, a]
            for yy in range(ny):
                @pl.when(y == yy)
                def _():
                    out_ref[a, 0] = now

                now = ydec[yy, a] * now + ybuf[yy, a, 0]
            pout[0, a] = now

            @pl.when(z < nz - 1)
            def _():
                up(a).start()

        @pl.when((b >= 0) & (b < heads))
        def _():
            ready(b, (2 * z > nz - 1))

            @pl.when(z < nz - 1)
            def _():
                down(b).wait_recv()

            now = pin[1, b]
            for yy in reversed(range(ny)):
                @pl.when(y == yy)
                def _():
                    out_ref[b, 1] = now

                now = ydec[yy, b] * now + ybuf[yy, b, 1]
            pout[1, b] = now

            @pl.when(z > 0)
            def _():
                down(b).start()

        @pl.when(t < pieces * (nz - 1))
        def _():
            hcopy(1 + t // pieces, t % pieces).start()

        return carry

    lax.fori_loop(0, max(heads + skew * (nz - 1), pieces * (nz - 1)), step, 0)

    for dz in range(1, nz):
        for p in range(pieces):
            harrive(dz, p).wait_recv()
        if halves == 2:
            share(dz, half).start()

    hcol_ref[pl.ds(pl.multiple_of(z * hland.shape[1], 128), hland.shape[1]), :] = (
        hid_f[:, pl.ds(pl.multiple_of(z * span, 128), span)].astype(BF16)
    )
    for dz in range(1, nz):
        there = (z + dz) % nz
        if halves == 2:
            share(dz, 1 - half).wait_recv()
        hcol_ref[pl.ds(pl.multiple_of(there * hland.shape[1], 128), hland.shape[1]), :] = hland[there].astype(BF16)
    for dz in range(1, nz):
        for p in range(pieces):
            hcopy(dz, p).wait_send()
        if halves == 2:
            share(dz, half).wait_send()
    for dy in range(1, ny):
        dcopy(dy).wait_send()

    def drain(h, carry):
        for dy in range(1, ny):
            ycopy(h, dy).wait_send()

        @pl.when(z < nz - 1)
        def _():
            up(h).wait_send()

        @pl.when(z > 0)
        def _():
            down(h).wait_send()

        return carry

    lax.fori_loop(0, heads, drain, 0)


def grads_kernel(ny, nz, ntp, width, gv_ref, hct_ref, ghp_ref, gw_ref, gh_ref,
                 gath, part, land, ghland,
                 upsend, dnsend, grecv, ysend, yrecv, hsend, hrecv):
    me = lax.axis_index("sp")
    mine = lax.axis_index("tp")
    z, y = me // ny, me % ny
    rows = gw_ref.shape[0]
    chunks = gv_ref.shape[1] // width
    length = gv_ref.shape[0]
    own_rows = gh_ref.shape[0]

    barrier = pltpu.get_barrier_semaphore()
    for dy in range(1, ny):
        pl.semaphore_signal(barrier, inc=1, device_id={"sp": z * ny + (y + dy) % ny}, device_id_type=MESH)
    for dz in (1, nz - 1):
        pl.semaphore_signal(barrier, inc=1, device_id={"sp": ((z + dz) % nz) * ny + y}, device_id_type=MESH)
    for dt in range(1, ntp):
        pl.semaphore_signal(barrier, inc=1, device_id={"tp": (mine + dt) % ntp}, device_id_type=MESH)
    pl.semaphore_wait(barrier, ny - 1 + 2 + ntp - 1)

    def cols(c):
        return pl.ds(pl.multiple_of(c * width, 128), width)

    def up(b, c):
        return remote(gath.at[b, c], gath.at[b, c], upsend.at[b, c], grecv.at[b, c], "sp", me + ny)

    def down(b, c):
        return remote(gath.at[b, c], gath.at[b, c], dnsend.at[b, c], grecv.at[b, c], "sp", me - ny)

    def launch(c, carry):
        gath[z, c] = gv_ref[:, cols(c)]

        @pl.when(z < nz - 1)
        def _():
            up(z, c).start()

        @pl.when(z > 0)
        def _():
            down(z, c).start()

        return carry

    lax.fori_loop(0, chunks, launch, 0)

    def hcopy(dt):
        there = (mine + dt) % ntp
        return remote(
            ghp_ref.at[pl.ds(pl.multiple_of(there * own_rows, 8), own_rows), :], ghland.at[mine],
            hsend.at[there], hrecv.at[mine], "tp", there,
        )

    def harrive(dt):
        there = (mine + dt) % ntp
        return remote(
            ghp_ref.at[pl.ds(pl.multiple_of(there * own_rows, 8), own_rows), :], ghland.at[there],
            hsend.at[there], hrecv.at[there], "tp", there,
        )

    for dt in range(1, ntp):
        hcopy(dt).start()

    def ycopy(c, there):
        return remote(
            part.at[there, c], land.at[y, c], ysend.at[there, c], yrecv.at[y, c], "sp", z * ny + there
        )

    def yarrive(c, there):
        return remote(
            part.at[there, c], land.at[there, c], ysend.at[there, c], yrecv.at[there, c], "sp", z * ny + there
        )

    def work(c, carry):
        for d in range(1, nz):
            low, high = z - d, z + d

            @pl.when(low >= 0)
            def _():
                down(jnp.maximum(low, 0), c).wait_recv()

                @pl.when(z < nz - 1)
                def _():
                    up(jnp.maximum(low, 0), c).start()

            @pl.when(high < nz)
            def _():
                up(jnp.minimum(high, nz - 1), c).wait_recv()

                @pl.when(z > 0)
                def _():
                    down(jnp.minimum(high, nz - 1), c).start()

        block = gath[:, c].reshape(nz * length, width).astype(BF16)
        for dy in range(1, ny):
            there = (y + dy) % ny
            part[there, c] = jnp.dot(
                hct_ref[pl.ds(pl.multiple_of(there * rows, 8), rows), :], block, preferred_element_type=F32
            )
            ycopy(c, there).start()
        gw_ref[:, cols(c)] = jnp.dot(
            hct_ref[pl.ds(pl.multiple_of(y * rows, 8), rows), :], block, preferred_element_type=F32
        )
        return carry

    lax.fori_loop(0, chunks, work, 0)

    total = ghp_ref[pl.ds(pl.multiple_of(mine * own_rows, 8), own_rows), :]
    for dt in range(1, ntp):
        harrive(dt).wait_recv()
        total = total + ghland[(mine + dt) % ntp]
    gh_ref[...] = total.astype(gh_ref.dtype)

    def collect(c, carry):
        for dy in range(1, ny):
            there = (y + dy) % ny
            yarrive(c, there).wait_recv()
            gw_ref[:, cols(c)] += land[there, c]
        return carry

    lax.fori_loop(0, chunks, collect, 0)

    def drain(c, carry):
        for dy in range(1, ny):
            ycopy(c, (y + dy) % ny).wait_send()
        for b in range(nz):
            @pl.when((b <= z) & (z < nz - 1))
            def _():
                up(b, c).wait_send()

            @pl.when((b >= z) & (z > 0))
            def _():
                down(b, c).wait_send()

        return carry

    lax.fori_loop(0, chunks, drain, 0)
    for dt in range(1, ntp):
        hcopy(dt).wait_send()


VM = pl.BlockSpec(memory_space=pltpu.VMEM)
LIMIT = 48 * 1024 * 1024


def split(x):
    hi = lax.reduce_precision(x, 8, 7)
    return hi.astype(BF16), (x - hi).astype(BF16)


def two_pass(spec, x, y):
    hi, lo = split(x)
    return jnp.einsum(spec, hi, y, preferred_element_type=F32) + jnp.einsum(spec, lo, y, preferred_element_type=F32)


def per_device(sp, tp, hidden, value_weight, key_vecs, queries, decay_pre, decay_rate, cotangent):
    length = hidden.shape[0]
    heads = decay_rate.shape[0]
    head_width = cotangent.shape[2]
    groups = key_vecs.shape[1]
    state = key_vecs.shape[2]
    per = heads // groups
    features = hidden.shape[1]
    columns = value_weight.shape[1]
    ny = inner_size(sp)
    nz = sp // ny
    values = jnp.dot(hidden, value_weight, preferred_element_type=F32).astype(BF16)
    v = values.reshape(length, groups, per, head_width)
    cot = cotangent.reshape(length, groups, per, head_width)
    log_decay = -decay_rate[None, :] * jax.nn.softplus(decay_pre)
    tri = jnp.tril(jnp.ones((length, length), F32))
    cum = jnp.dot(tri, log_decay, precision=lax.Precision.HIGHEST)
    tot = cum[-1]
    to_end = jnp.exp(tot[None] - cum).reshape(length, groups, per, 1)
    ecum = jnp.exp(cum).reshape(length, groups, per, 1)
    local_state = two_pass("sgip,sgn->gipn", to_end * v.astype(F32), key_vecs)
    local_pull = two_pass("sgip,sgn->gipn", ecum * cot.astype(F32), queries)
    both = jnp.stack([local_state, local_pull], axis=2).reshape(heads, 2, head_width, state)
    dec = jnp.broadcast_to(jnp.exp(tot)[:, None, None], (heads, 1, state))
    span = features // nz
    pieces = 4
    scanned, hcol = pl.pallas_call(
        functools.partial(scan_kernel, ny, nz, tp, 3, pieces),
        out_shape=(
            jax.ShapeDtypeStruct(both.shape, F32),
            jax.ShapeDtypeStruct((nz * length, span), BF16),
        ),
        in_specs=[VM] * 3,
        out_specs=(VM, VM),
        scratch_shapes=[
            pltpu.VMEM((ny,) + both.shape, F32),
            pltpu.VMEM((ny,) + dec.shape, F32),
            pltpu.VMEM((2, heads, head_width, state), F32),
            pltpu.VMEM((2, heads, head_width, state), F32),
            pltpu.VMEM((length, features), F32),
            pltpu.VMEM((nz, length, span), F32),
            pltpu.SemaphoreType.DMA((ny, heads)),
            pltpu.SemaphoreType.DMA((ny, heads)),
            pltpu.SemaphoreType.DMA((ny,)),
            pltpu.SemaphoreType.DMA((ny,)),
            pltpu.SemaphoreType.DMA((2, heads)),
            pltpu.SemaphoreType.DMA((2, heads)),
            pltpu.SemaphoreType.DMA((nz, pieces)),
            pltpu.SemaphoreType.DMA((nz, pieces)),
            pltpu.SemaphoreType.DMA((nz,)),
            pltpu.SemaphoreType.DMA((nz,)),
        ],
        compiler_params=pltpu.CompilerParams(collective_id=0, has_side_effects=True, vmem_limit_bytes=LIMIT),
        name="scan_states",
    )(both, dec, hidden)
    state_in = scanned[:, 0].reshape(groups, per, head_width, state)
    state_grad = scanned[:, 1].reshape(groups, per, head_width, state)

    cum_h = cum.T
    causal = jnp.tril(jnp.ones((length, length), dtype=bool))[None]
    across = cum_h[:, :, None] - cum_h[:, None, :]
    damping = jnp.where(causal, jnp.exp(jnp.where(causal, across, 0.0)), 0.0).reshape(groups, per, length, length)
    scores = jnp.einsum("tgn,sgn->gts", queries, key_vecs, preferred_element_type=F32)
    pair = jnp.einsum("tgip,sgip->gits", cot, v, preferred_element_type=F32)
    dscore = pair * damping
    flux = dscore * scores[:, None]
    net = (jnp.sum(flux, axis=3) - jnp.sum(flux, axis=2)).reshape(heads, length).T
    dsum = jnp.sum(dscore, axis=1)
    mixed = scores[:, None] * damping
    gq_heads = ecum * two_pass("gipn,tgip->tgin", state_in, cot)
    gk_heads = to_end * two_pass("gipn,tgip->tgin", state_grad, v)
    gv = two_pass("gits,tgip->sgip", mixed, cot) + to_end * two_pass(
        "gipn,sgn->sgip", state_grad, key_vecs
    )
    gq = two_pass("gts,sgn->tgn", dsum, key_vecs) + jnp.sum(gq_heads, axis=2)
    gk = two_pass("gts,tgn->sgn", dsum, queries) + jnp.sum(gk_heads, axis=2)
    qgq = jnp.sum(gq_heads * queries.astype(F32)[:, :, None], axis=3).reshape(length, heads)
    kgk = jnp.sum(gk_heads * key_vecs.astype(F32)[:, :, None], axis=3).reshape(length, heads)
    through = jnp.exp(tot) * jnp.sum(state_in * state_grad, axis=(2, 3)).reshape(heads)
    suffix = jnp.dot(tri.T, net + qgq, precision=lax.Precision.HIGHEST)
    prefix = jnp.dot(tri - jnp.eye(length, dtype=F32), kgk, precision=lax.Precision.HIGHEST)
    grad_decay = (suffix + prefix + through[None]) * -decay_rate[None] * jax.nn.sigmoid(decay_pre)

    grad_flat = gv.reshape(length, columns).astype(BF16)
    ghp = lax.dot_general(grad_flat, value_weight, (((1,), (1,)), ((), ())), preferred_element_type=F32)
    rows = features // sp
    width = min(columns, 128)
    chunks = columns // width
    grad_weight, grad_hidden = pl.pallas_call(
        functools.partial(grads_kernel, ny, nz, tp, width),
        out_shape=(
            jax.ShapeDtypeStruct((rows, columns), F32),
            jax.ShapeDtypeStruct((length // tp, features), BF16),
        ),
        in_specs=[VM] * 3,
        out_specs=(VM, VM),
        scratch_shapes=[
            pltpu.VMEM((nz, chunks, length, width), F32),
            pltpu.VMEM((ny, chunks, rows, width), F32),
            pltpu.VMEM((ny, chunks, rows, width), F32),
            pltpu.VMEM((tp, length // tp, features), F32),
            pltpu.SemaphoreType.DMA((nz, chunks)),
            pltpu.SemaphoreType.DMA((nz, chunks)),
            pltpu.SemaphoreType.DMA((nz, chunks)),
            pltpu.SemaphoreType.DMA((ny, chunks)),
            pltpu.SemaphoreType.DMA((ny, chunks)),
            pltpu.SemaphoreType.DMA((tp,)),
            pltpu.SemaphoreType.DMA((tp,)),
        ],
        compiler_params=pltpu.CompilerParams(collective_id=1, has_side_effects=True, vmem_limit_bytes=LIMIT),
        name="weight_grads",
    )(grad_flat.astype(F32), hcol.T, ghp)
    return (gq_cast(gk), gq_cast(gq), grad_decay, grad_hidden, grad_weight)


def gq_cast(x):
    return x.astype(BF16)


def solution(mesh):
    return jax.shard_map(
        functools.partial(per_device, mesh.shape["sp"], mesh.shape["tp"]),
        mesh=mesh,
        in_specs=(
            P("sp", None),
            P(None, "tp"),
            P("sp", "tp", None),
            P("sp", "tp", None),
            P("sp", "tp"),
            P("tp"),
            P("sp", "tp", None),
        ),
        out_specs=(
            P("sp", "tp", None),
            P("sp", "tp", None),
            P("sp", "tp"),
            P(("sp", "tp"), None),
            P("sp", "tp"),
        ),
        check_vma=False,
    )
```

```python
import functools

import jax
import jax.numpy as jnp
from jax import lax
from jax.experimental import pallas as pl
from jax.experimental.pallas import tpu as pltpu
from jax.sharding import PartitionSpec as P

MESH = pl.DeviceIdType.MESH
F32 = jnp.float32
BF16 = jnp.bfloat16


def inner_size(count):
    size = 1
    while size * size * 4 <= count:
        size *= 2
    while count % size:
        size -= 1
    return size


def remote(src, dst, send, recv, axis, index):
    return pltpu.make_async_remote_copy(
        src_ref=src, dst_ref=dst, send_sem=send, recv_sem=recv, device_id={axis: index}, device_id_type=MESH
    )


def scan_kernel(ny, nz, ntp, skew, pieces, both_ref, dec_ref, hid_ref, out_ref, hcol_ref,
                ybuf, ydec, pin, pout, hid_f, hland,
                ysend, yrecv, dsend, drecv, psend, precv, hsend, hrecv, fsend, frecv):
    me = lax.axis_index("sp")
    z, y = me // ny, me % ny
    heads = both_ref.shape[0]
    span = hland.shape[2]

    barrier = pltpu.get_barrier_semaphore()
    for dy in range(1, ny):
        pl.semaphore_signal(barrier, inc=1, device_id={"sp": z * ny + (y + dy) % ny}, device_id_type=MESH)
    for dz in range(1, nz):
        pl.semaphore_signal(barrier, inc=1, device_id={"sp": ((z + dz) % nz) * ny + y}, device_id_type=MESH)
    mine = lax.axis_index("tp")
    halves = 2 if ntp % 2 == 0 else 1
    half = mine % halves
    other = mine + 1 - 2 * half
    if halves == 2:
        pl.semaphore_signal(barrier, inc=1, device_id={"tp": other}, device_id_type=MESH)
    pl.semaphore_wait(barrier, ny - 1 + nz - 1 + halves - 1)
    half_rows = hland.shape[1] // halves
    piece_rows = half_rows // pieces

    def ycopy(h, dy):
        there = (y + dy) % ny
        return remote(both_ref.at[h], ybuf.at[y, h], ysend.at[there, h], yrecv.at[y, h], "sp", z * ny + there)

    def yarrive(h, there):
        return remote(both_ref.at[h], ybuf.at[there, h], ysend.at[there, h], yrecv.at[there, h], "sp", z * ny + there)

    def dcopy(dy):
        there = (y + dy) % ny
        return remote(dec_ref, ydec.at[y], dsend.at[there], drecv.at[y], "sp", z * ny + there)

    def darrive(dy):
        there = (y + dy) % ny
        return remote(dec_ref, ydec.at[there], dsend.at[there], drecv.at[there], "sp", z * ny + there)

    for dy in range(1, ny):
        dcopy(dy).start()

    def launch(h, carry):
        for dy in range(1, ny):
            ycopy(h, dy).start()
        return carry

    lax.fori_loop(0, heads, launch, 0)

    def piece(p):
        return pl.ds(pl.multiple_of(half * half_rows + p * piece_rows, 8), piece_rows)

    def columns_of(plane):
        return pl.ds(pl.multiple_of(plane * span, 128), span)

    def hcopy(dz, p):
        there = (z + dz) % nz
        return remote(
            hid_f.at[piece(p), columns_of(there)], hland.at[z, piece(p)],
            hsend.at[there, p], hrecv.at[z, p], "sp", there * ny + y,
        )

    def harrive(dz, p):
        there = (z + dz) % nz
        return remote(
            hid_f.at[piece(p), columns_of(there)], hland.at[there, piece(p)],
            hsend.at[there, p], hrecv.at[there, p], "sp", there * ny + y,
        )

    def share(dz, part):
        there = (z + dz) % nz
        block = hland.at[there, pl.ds(pl.multiple_of(part * half_rows, 8), half_rows)]
        return remote(block, block, fsend.at[there], frecv.at[there], "tp", other)

    hid_f[...] = hid_ref[...].astype(F32)
    ybuf[y] = both_ref[...]
    ydec[y] = dec_ref[...]
    for dy in range(1, ny):
        darrive(dy).wait_recv()

    @pl.when(z == 0)
    def _():
        pin[0] = jnp.zeros_like(pin[0])

    @pl.when(z == nz - 1)
    def _():
        pin[1] = jnp.zeros_like(pin[1])

    def up(h):
        return remote(pout.at[0, h], pin.at[0, h], psend.at[0, h], precv.at[0, h], "sp", me + ny)

    def down(h):
        return remote(pout.at[1, h], pin.at[1, h], psend.at[1, h], precv.at[1, h], "sp", me - ny)

    def ready(h, first):
        @pl.when(first)
        def _():
            for dy in range(1, ny):
                yarrive(h, (y + dy) % ny).wait_recv()

    def step(t, carry):
        a = t - skew * z
        b = t - skew * (nz - 1 - z)

        @pl.when((a >= 0) & (a < heads))
        def _():
            ready(a, (2 * z <= nz - 1))

            @pl.when(z > 0)
            def _():
                up(a).wait_recv()

            now = pin[0, a]
            for yy in range(ny):
                @pl.when(y == yy)
                def _():
                    out_ref[a, 0] = now

                now = ydec[yy, a] * now + ybuf[yy, a, 0]
            pout[0, a] = now

            @pl.when(z < nz - 1)
            def _():
                up(a).start()

        @pl.when((b >= 0) & (b < heads))
        def _():
            ready(b, (2 * z > nz - 1))

            @pl.when(z < nz - 1)
            def _():
                down(b).wait_recv()

            now = pin[1, b]
            for yy in reversed(range(ny)):
                @pl.when(y == yy)
                def _():
                    out_ref[b, 1] = now

                now = ydec[yy, b] * now + ybuf[yy, b, 1]
            pout[1, b] = now

            @pl.when(z > 0)
            def _():
                down(b).start()

        @pl.when(t < pieces * (nz - 1))
        def _():
            hcopy(1 + t // pieces, t % pieces).start()

        return carry

    lax.fori_loop(0, max(heads + skew * (nz - 1), pieces * (nz - 1)), step, 0)

    for dz in range(1, nz):
        for p in range(pieces):
            harrive(dz, p).wait_recv()
        if halves == 2:
            share(dz, half).start()

    hcol_ref[pl.ds(pl.multiple_of(z * hland.shape[1], 128), hland.shape[1]), :] = (
        hid_f[:, pl.ds(pl.multiple_of(z * span, 128), span)].astype(BF16)
    )
    for dz in range(1, nz):
        there = (z + dz) % nz
        if halves == 2:
            share(dz, 1 - half).wait_recv()
        hcol_ref[pl.ds(pl.multiple_of(there * hland.shape[1], 128), hland.shape[1]), :] = hland[there].astype(BF16)
    for dz in range(1, nz):
        for p in range(pieces):
            hcopy(dz, p).wait_send()
        if halves == 2:
            share(dz, half).wait_send()
    for dy in range(1, ny):
        dcopy(dy).wait_send()

    def drain(h, carry):
        for dy in range(1, ny):
            ycopy(h, dy).wait_send()

        @pl.when(z < nz - 1)
        def _():
            up(h).wait_send()

        @pl.when(z > 0)
        def _():
            down(h).wait_send()

        return carry

    lax.fori_loop(0, heads, drain, 0)


def grads_kernel(ny, nz, ntp, width, gv_ref, hct_ref, ghp_ref, gw_ref, gh_ref,
                 gath, part, land, ghland,
                 upsend, dnsend, grecv, ysend, yrecv, hsend, hrecv):
    me = lax.axis_index("sp")
    mine = lax.axis_index("tp")
    z, y = me // ny, me % ny
    rows = gw_ref.shape[0]
    chunks = gv_ref.shape[1] // width
    length = gv_ref.shape[0]
    own_rows = gh_ref.shape[0]

    barrier = pltpu.get_barrier_semaphore()
    for dy in range(1, ny):
        pl.semaphore_signal(barrier, inc=1, device_id={"sp": z * ny + (y + dy) % ny}, device_id_type=MESH)
    for dz in (1, nz - 1):
        pl.semaphore_signal(barrier, inc=1, device_id={"sp": ((z + dz) % nz) * ny + y}, device_id_type=MESH)
    for dt in range(1, ntp):
        pl.semaphore_signal(barrier, inc=1, device_id={"tp": (mine + dt) % ntp}, device_id_type=MESH)
    pl.semaphore_wait(barrier, ny - 1 + 2 + ntp - 1)

    def cols(c):
        return pl.ds(pl.multiple_of(c * width, 128), width)

    def up(b, c):
        return remote(gath.at[b, c], gath.at[b, c], upsend.at[b, c], grecv.at[b, c], "sp", me + ny)

    def down(b, c):
        return remote(gath.at[b, c], gath.at[b, c], dnsend.at[b, c], grecv.at[b, c], "sp", me - ny)

    def launch(c, carry):
        gath[z, c] = gv_ref[:, cols(c)]

        @pl.when(z < nz - 1)
        def _():
            up(z, c).start()

        @pl.when(z > 0)
        def _():
            down(z, c).start()

        return carry

    ahead = min(2, chunks)
    lax.fori_loop(0, ahead, launch, 0)

    def hcopy(dt):
        there = (mine + dt) % ntp
        return remote(
            ghp_ref.at[pl.ds(pl.multiple_of(there * own_rows, 8), own_rows), :], ghland.at[mine],
            hsend.at[there], hrecv.at[mine], "tp", there,
        )

    def harrive(dt):
        there = (mine + dt) % ntp
        return remote(
            ghp_ref.at[pl.ds(pl.multiple_of(there * own_rows, 8), own_rows), :], ghland.at[there],
            hsend.at[there], hrecv.at[there], "tp", there,
        )

    for dt in range(1, ntp):
        hcopy(dt).start()

    def ycopy(c, there):
        return remote(
            part.at[there, c], land.at[y, c], ysend.at[there, c], yrecv.at[y, c], "sp", z * ny + there
        )

    def yarrive(c, there):
        return remote(
            part.at[there, c], land.at[there, c], ysend.at[there, c], yrecv.at[there, c], "sp", z * ny + there
        )

    def work(c, carry):
        for d in range(1, nz):
            low, high = z - d, z + d

            @pl.when(low >= 0)
            def _():
                down(jnp.maximum(low, 0), c).wait_recv()

                @pl.when(z < nz - 1)
                def _():
                    up(jnp.maximum(low, 0), c).start()

            @pl.when(high < nz)
            def _():
                up(jnp.minimum(high, nz - 1), c).wait_recv()

                @pl.when(z > 0)
                def _():
                    down(jnp.minimum(high, nz - 1), c).start()

        @pl.when(c + ahead < chunks)
        def _():
            launch(c + ahead, 0)

        block = gath[:, c].reshape(nz * length, width).astype(BF16)
        for dy in range(1, ny):
            there = (y + dy) % ny
            part[there, c] = jnp.dot(
                hct_ref[pl.ds(pl.multiple_of(there * rows, 8), rows), :], block, preferred_element_type=F32
            )
            ycopy(c, there).start()
        gw_ref[:, cols(c)] = jnp.dot(
            hct_ref[pl.ds(pl.multiple_of(y * rows, 8), rows), :], block, preferred_element_type=F32
        )
        return carry

    lax.fori_loop(0, chunks, work, 0)

    total = ghp_ref[pl.ds(pl.multiple_of(mine * own_rows, 8), own_rows), :]
    for dt in range(1, ntp):
        harrive(dt).wait_recv()
        total = total + ghland[(mine + dt) % ntp]
    gh_ref[...] = total.astype(gh_ref.dtype)

    def collect(c, carry):
        for dy in range(1, ny):
            there = (y + dy) % ny
            yarrive(c, there).wait_recv()
            gw_ref[:, cols(c)] += land[there, c]
        return carry

    lax.fori_loop(0, chunks, collect, 0)

    def drain(c, carry):
        for dy in range(1, ny):
            ycopy(c, (y + dy) % ny).wait_send()
        for b in range(nz):
            @pl.when((b <= z) & (z < nz - 1))
            def _():
                up(b, c).wait_send()

            @pl.when((b >= z) & (z > 0))
            def _():
                down(b, c).wait_send()

        return carry

    lax.fori_loop(0, chunks, drain, 0)
    for dt in range(1, ntp):
        hcopy(dt).wait_send()


VM = pl.BlockSpec(memory_space=pltpu.VMEM)
LIMIT = 48 * 1024 * 1024


def split(x):
    hi = lax.reduce_precision(x, 8, 7)
    return hi.astype(BF16), (x - hi).astype(BF16)


def two_pass(spec, x, y):
    hi, lo = split(x)
    return jnp.einsum(spec, hi, y, preferred_element_type=F32) + jnp.einsum(spec, lo, y, preferred_element_type=F32)


def per_device(sp, tp, hidden, value_weight, key_vecs, queries, decay_pre, decay_rate, cotangent):
    length = hidden.shape[0]
    heads = decay_rate.shape[0]
    head_width = cotangent.shape[2]
    groups = key_vecs.shape[1]
    state = key_vecs.shape[2]
    per = heads // groups
    features = hidden.shape[1]
    columns = value_weight.shape[1]
    ny = inner_size(sp)
    nz = sp // ny
    values = jnp.dot(hidden, value_weight, preferred_element_type=F32).astype(BF16)
    v = values.reshape(length, groups, per, head_width)
    cot = cotangent.reshape(length, groups, per, head_width)
    log_decay = -decay_rate[None, :] * jax.nn.softplus(decay_pre)
    tri = jnp.tril(jnp.ones((length, length), F32))
    cum = jnp.dot(tri, log_decay, precision=lax.Precision.HIGHEST)
    tot = cum[-1]
    to_end = jnp.exp(tot[None] - cum).reshape(length, groups, per, 1)
    ecum = jnp.exp(cum).reshape(length, groups, per, 1)
    local_state = two_pass("sgip,sgn->gipn", to_end * v.astype(F32), key_vecs)
    local_pull = two_pass("sgip,sgn->gipn", ecum * cot.astype(F32), queries)
    both = jnp.stack([local_state, local_pull], axis=2).reshape(heads, 2, head_width, state)
    dec = jnp.broadcast_to(jnp.exp(tot)[:, None, None], (heads, 1, state))
    span = features // nz
    pieces = 4
    scanned, hcol = pl.pallas_call(
        functools.partial(scan_kernel, ny, nz, tp, 2, pieces),
        out_shape=(
            jax.ShapeDtypeStruct(both.shape, F32),
            jax.ShapeDtypeStruct((nz * length, span), BF16),
        ),
        in_specs=[VM] * 3,
        out_specs=(VM, VM),
        scratch_shapes=[
            pltpu.VMEM((ny,) + both.shape, F32),
            pltpu.VMEM((ny,) + dec.shape, F32),
            pltpu.VMEM((2, heads, head_width, state), F32),
            pltpu.VMEM((2, heads, head_width, state), F32),
            pltpu.VMEM((length, features), F32),
            pltpu.VMEM((nz, length, span), F32),
            pltpu.SemaphoreType.DMA((ny, heads)),
            pltpu.SemaphoreType.DMA((ny, heads)),
            pltpu.SemaphoreType.DMA((ny,)),
            pltpu.SemaphoreType.DMA((ny,)),
            pltpu.SemaphoreType.DMA((2, heads)),
            pltpu.SemaphoreType.DMA((2, heads)),
            pltpu.SemaphoreType.DMA((nz, pieces)),
            pltpu.SemaphoreType.DMA((nz, pieces)),
            pltpu.SemaphoreType.DMA((nz,)),
            pltpu.SemaphoreType.DMA((nz,)),
        ],
        compiler_params=pltpu.CompilerParams(collective_id=0, has_side_effects=True, vmem_limit_bytes=LIMIT),
        name="scan_states",
    )(both, dec, hidden)
    state_in = scanned[:, 0].reshape(groups, per, head_width, state)
    state_grad = scanned[:, 1].reshape(groups, per, head_width, state)

    cum_h = cum.T
    causal = jnp.tril(jnp.ones((length, length), dtype=bool))[None]
    across = cum_h[:, :, None] - cum_h[:, None, :]
    damping = jnp.where(causal, jnp.exp(jnp.where(causal, across, 0.0)), 0.0).reshape(groups, per, length, length)
    scores = jnp.einsum("tgn,sgn->gts", queries, key_vecs, preferred_element_type=F32)
    pair = jnp.einsum("tgip,sgip->gits", cot, v, preferred_element_type=F32)
    dscore = pair * damping
    flux = dscore * scores[:, None]
    net = (jnp.sum(flux, axis=3) - jnp.sum(flux, axis=2)).reshape(heads, length).T
    dsum = jnp.sum(dscore, axis=1)
    mixed = scores[:, None] * damping
    gq_heads = ecum * two_pass("gipn,tgip->tgin", state_in, cot)
    gk_heads = to_end * two_pass("gipn,tgip->tgin", state_grad, v)
    gv = two_pass("gits,tgip->sgip", mixed, cot) + to_end * two_pass(
        "gipn,sgn->sgip", state_grad, key_vecs
    )
    gq = two_pass("gts,sgn->tgn", dsum, key_vecs) + jnp.sum(gq_heads, axis=2)
    gk = two_pass("gts,tgn->sgn", dsum, queries) + jnp.sum(gk_heads, axis=2)
    qgq = jnp.sum(gq_heads * queries.astype(F32)[:, :, None], axis=3).reshape(length, heads)
    kgk = jnp.sum(gk_heads * key_vecs.astype(F32)[:, :, None], axis=3).reshape(length, heads)
    through = jnp.exp(tot) * jnp.sum(state_in * state_grad, axis=(2, 3)).reshape(heads)
    suffix = jnp.dot(tri.T, net + qgq, precision=lax.Precision.HIGHEST)
    prefix = jnp.dot(tri - jnp.eye(length, dtype=F32), kgk, precision=lax.Precision.HIGHEST)
    grad_decay = (suffix + prefix + through[None]) * -decay_rate[None] * jax.nn.sigmoid(decay_pre)

    grad_flat = gv.reshape(length, columns).astype(BF16)
    ghp = lax.dot_general(grad_flat, value_weight, (((1,), (1,)), ((), ())), preferred_element_type=F32)
    rows = features // sp
    width = min(columns, 128)
    chunks = columns // width
    grad_weight, grad_hidden = pl.pallas_call(
        functools.partial(grads_kernel, ny, nz, tp, width),
        out_shape=(
            jax.ShapeDtypeStruct((rows, columns), F32),
            jax.ShapeDtypeStruct((length // tp, features), BF16),
        ),
        in_specs=[VM] * 3,
        out_specs=(VM, VM),
        scratch_shapes=[
            pltpu.VMEM((nz, chunks, length, width), F32),
            pltpu.VMEM((ny, chunks, rows, width), F32),
            pltpu.VMEM((ny, chunks, rows, width), F32),
            pltpu.VMEM((tp, length // tp, features), F32),
            pltpu.SemaphoreType.DMA((nz, chunks)),
            pltpu.SemaphoreType.DMA((nz, chunks)),
            pltpu.SemaphoreType.DMA((nz, chunks)),
            pltpu.SemaphoreType.DMA((ny, chunks)),
            pltpu.SemaphoreType.DMA((ny, chunks)),
            pltpu.SemaphoreType.DMA((tp,)),
            pltpu.SemaphoreType.DMA((tp,)),
        ],
        compiler_params=pltpu.CompilerParams(collective_id=1, has_side_effects=True, vmem_limit_bytes=LIMIT),
        name="weight_grads",
    )(grad_flat.astype(F32), hcol.T, ghp)
    return (gq_cast(gk), gq_cast(gq), grad_decay, grad_hidden, grad_weight)


def gq_cast(x):
    return x.astype(BF16)


def solution(mesh):
    return jax.shard_map(
        functools.partial(per_device, mesh.shape["sp"], mesh.shape["tp"]),
        mesh=mesh,
        in_specs=(
            P("sp", None),
            P(None, "tp"),
            P("sp", "tp", None),
            P("sp", "tp", None),
            P("sp", "tp"),
            P("tp"),
            P("sp", "tp", None),
        ),
        out_specs=(
            P("sp", "tp", None),
            P("sp", "tp", None),
            P("sp", "tp"),
            P(("sp", "tp"), None),
            P("sp", "tp"),
        ),
        check_vma=False,
    )
```

```python
import functools

import jax
import jax.numpy as jnp
from jax import lax
from jax.experimental import pallas as pl
from jax.experimental.pallas import tpu as pltpu
from jax.sharding import PartitionSpec as P

MESH = pl.DeviceIdType.MESH
F32 = jnp.float32
BF16 = jnp.bfloat16


def inner_size(count):
    size = 1
    while size * size * 4 <= count:
        size *= 2
    while count % size:
        size -= 1
    return size


def remote(src, dst, send, recv, axis, index):
    return pltpu.make_async_remote_copy(
        src_ref=src, dst_ref=dst, send_sem=send, recv_sem=recv, device_id={axis: index}, device_id_type=MESH
    )


def scan_kernel(ny, nz, ntp, skew, pieces, both_ref, dec_ref, hid_ref, out_ref, hcol_ref,
                ybuf, ydec, pin, pout, hid_f, hland,
                ysend, yrecv, dsend, drecv, psend, precv, hsend, hrecv, fsend, frecv):
    me = lax.axis_index("sp")
    z, y = me // ny, me % ny
    heads = both_ref.shape[0]
    span = hland.shape[2]

    barrier = pltpu.get_barrier_semaphore()
    for dy in range(1, ny):
        pl.semaphore_signal(barrier, inc=1, device_id={"sp": z * ny + (y + dy) % ny}, device_id_type=MESH)
    for dz in range(1, nz):
        pl.semaphore_signal(barrier, inc=1, device_id={"sp": ((z + dz) % nz) * ny + y}, device_id_type=MESH)
    mine = lax.axis_index("tp")
    halves = 2 if ntp % 2 == 0 else 1
    half = mine % halves
    other = mine + 1 - 2 * half
    if halves == 2:
        pl.semaphore_signal(barrier, inc=1, device_id={"tp": other}, device_id_type=MESH)
    pl.semaphore_wait(barrier, ny - 1 + nz - 1 + halves - 1)
    half_rows = hland.shape[1] // halves
    piece_rows = half_rows // pieces

    def ycopy(h, dy):
        there = (y + dy) % ny
        return remote(both_ref.at[h], ybuf.at[y, h], ysend.at[there, h], yrecv.at[y, h], "sp", z * ny + there)

    def yarrive(h, there):
        return remote(both_ref.at[h], ybuf.at[there, h], ysend.at[there, h], yrecv.at[there, h], "sp", z * ny + there)

    def dcopy(dy):
        there = (y + dy) % ny
        return remote(dec_ref, ydec.at[y], dsend.at[there], drecv.at[y], "sp", z * ny + there)

    def darrive(dy):
        there = (y + dy) % ny
        return remote(dec_ref, ydec.at[there], dsend.at[there], drecv.at[there], "sp", z * ny + there)

    for dy in range(1, ny):
        dcopy(dy).start()

    def launch(h, carry):
        for dy in range(1, ny):
            ycopy(h, dy).start()
        return carry

    lax.fori_loop(0, heads, launch, 0)

    def piece(p):
        return pl.ds(pl.multiple_of(half * half_rows + p * piece_rows, 8), piece_rows)

    def columns_of(plane):
        return pl.ds(pl.multiple_of(plane * span, 128), span)

    def hcopy(dz, p):
        there = (z + dz) % nz
        return remote(
            hid_f.at[piece(p), columns_of(there)], hland.at[z, piece(p)],
            hsend.at[there, p], hrecv.at[z, p], "sp", there * ny + y,
        )

    def harrive(dz, p):
        there = (z + dz) % nz
        return remote(
            hid_f.at[piece(p), columns_of(there)], hland.at[there, piece(p)],
            hsend.at[there, p], hrecv.at[there, p], "sp", there * ny + y,
        )

    def share(dz, part):
        there = (z + dz) % nz
        block = hland.at[there, pl.ds(pl.multiple_of(part * half_rows, 8), half_rows)]
        return remote(block, block, fsend.at[there], frecv.at[there], "tp", other)

    hid_f[...] = hid_ref[...].astype(F32)
    ybuf[y] = both_ref[...]
    ydec[y] = dec_ref[...]
    for dy in range(1, ny):
        darrive(dy).wait_recv()

    @pl.when(z == 0)
    def _():
        pin[0] = jnp.zeros_like(pin[0])

    @pl.when(z == nz - 1)
    def _():
        pin[1] = jnp.zeros_like(pin[1])

    def up(h):
        return remote(pout.at[0, h], pin.at[0, h], psend.at[0, h], precv.at[0, h], "sp", me + ny)

    def down(h):
        return remote(pout.at[1, h], pin.at[1, h], psend.at[1, h], precv.at[1, h], "sp", me - ny)

    def ready(h, first):
        @pl.when(first)
        def _():
            for dy in range(1, ny):
                yarrive(h, (y + dy) % ny).wait_recv()

    def step(t, carry):
        a = t - skew * z
        b = t - skew * (nz - 1 - z)

        @pl.when((a >= 0) & (a < heads))
        def _():
            ready(a, (2 * z <= nz - 1))

            @pl.when(z > 0)
            def _():
                up(a).wait_recv()

            now = pin[0, a]
            for yy in range(ny):
                @pl.when(y == yy)
                def _():
                    out_ref[a, 0] = now

                now = ydec[yy, a] * now + ybuf[yy, a, 0]
            pout[0, a] = now

            @pl.when(z < nz - 1)
            def _():
                up(a).start()

        @pl.when((b >= 0) & (b < heads))
        def _():
            ready(b, (2 * z > nz - 1))

            @pl.when(z < nz - 1)
            def _():
                down(b).wait_recv()

            now = pin[1, b]
            for yy in reversed(range(ny)):
                @pl.when(y == yy)
                def _():
                    out_ref[b, 1] = now

                now = ydec[yy, b] * now + ybuf[yy, b, 1]
            pout[1, b] = now

            @pl.when(z > 0)
            def _():
                down(b).start()

        @pl.when(t < pieces * (nz - 1))
        def _():
            hcopy(1 + t // pieces, t % pieces).start()

        return carry

    lax.fori_loop(0, max(heads + skew * (nz - 1), pieces * (nz - 1)), step, 0)

    for dz in range(1, nz):
        for p in range(pieces):
            harrive(dz, p).wait_recv()
        if halves == 2:
            share(dz, half).start()

    hcol_ref[pl.ds(pl.multiple_of(z * hland.shape[1], 128), hland.shape[1]), :] = (
        hid_f[:, pl.ds(pl.multiple_of(z * span, 128), span)].astype(BF16)
    )
    for dz in range(1, nz):
        there = (z + dz) % nz
        if halves == 2:
            share(dz, 1 - half).wait_recv()
        hcol_ref[pl.ds(pl.multiple_of(there * hland.shape[1], 128), hland.shape[1]), :] = hland[there].astype(BF16)
    for dz in range(1, nz):
        for p in range(pieces):
            hcopy(dz, p).wait_send()
        if halves == 2:
            share(dz, half).wait_send()
    for dy in range(1, ny):
        dcopy(dy).wait_send()

    def drain(h, carry):
        for dy in range(1, ny):
            ycopy(h, dy).wait_send()

        @pl.when(z < nz - 1)
        def _():
            up(h).wait_send()

        @pl.when(z > 0)
        def _():
            down(h).wait_send()

        return carry

    lax.fori_loop(0, heads, drain, 0)


def grads_kernel(ny, nz, ntp, width, gv_ref, hct_ref, ghp_ref, gw_ref, gh_ref,
                 gath, part, land, ghland,
                 upsend, dnsend, grecv, ysend, yrecv, hsend, hrecv):
    me = lax.axis_index("sp")
    mine = lax.axis_index("tp")
    z, y = me // ny, me % ny
    rows = gw_ref.shape[0]
    chunks = gv_ref.shape[1] // width
    length = gv_ref.shape[0]
    own_rows = gh_ref.shape[0]

    barrier = pltpu.get_barrier_semaphore()
    for dy in range(1, ny):
        pl.semaphore_signal(barrier, inc=1, device_id={"sp": z * ny + (y + dy) % ny}, device_id_type=MESH)
    for dz in (1, nz - 1):
        pl.semaphore_signal(barrier, inc=1, device_id={"sp": ((z + dz) % nz) * ny + y}, device_id_type=MESH)
    for dt in range(1, ntp):
        pl.semaphore_signal(barrier, inc=1, device_id={"tp": (mine + dt) % ntp}, device_id_type=MESH)
    pl.semaphore_wait(barrier, ny - 1 + 2 + ntp - 1)

    def cols(c):
        return pl.ds(pl.multiple_of(c * width, 128), width)

    def up(b, c):
        return remote(gath.at[b, c], gath.at[b, c], upsend.at[b, c], grecv.at[b, c], "sp", me + ny)

    def down(b, c):
        return remote(gath.at[b, c], gath.at[b, c], dnsend.at[b, c], grecv.at[b, c], "sp", me - ny)

    def launch(c, carry):
        gath[z, c] = gv_ref[:, cols(c)]

        @pl.when(z < nz - 1)
        def _():
            up(z, c).start()

        @pl.when(z > 0)
        def _():
            down(z, c).start()

        return carry

    ahead = min(5, chunks)
    lax.fori_loop(0, ahead, launch, 0)

    def hcopy(dt):
        there = (mine + dt) % ntp
        return remote(
            ghp_ref.at[pl.ds(pl.multiple_of(there * own_rows, 8), own_rows), :], ghland.at[mine],
            hsend.at[there], hrecv.at[mine], "tp", there,
        )

    def harrive(dt):
        there = (mine + dt) % ntp
        return remote(
            ghp_ref.at[pl.ds(pl.multiple_of(there * own_rows, 8), own_rows), :], ghland.at[there],
            hsend.at[there], hrecv.at[there], "tp", there,
        )

    for dt in range(1, ntp):
        hcopy(dt).start()

    def ycopy(c, there):
        return remote(
            part.at[there, c], land.at[y, c], ysend.at[there, c], yrecv.at[y, c], "sp", z * ny + there
        )

    def yarrive(c, there):
        return remote(
            part.at[there, c], land.at[there, c], ysend.at[there, c], yrecv.at[there, c], "sp", z * ny + there
        )

    def work(c, carry):
        for d in range(1, nz):
            low, high = z - d, z + d

            @pl.when(low >= 0)
            def _():
                down(jnp.maximum(low, 0), c).wait_recv()

                @pl.when(z < nz - 1)
                def _():
                    up(jnp.maximum(low, 0), c).start()

            @pl.when(high < nz)
            def _():
                up(jnp.minimum(high, nz - 1), c).wait_recv()

                @pl.when(z > 0)
                def _():
                    down(jnp.minimum(high, nz - 1), c).start()

        @pl.when(c + ahead < chunks)
        def _():
            launch(c + ahead, 0)

        block = gath[:, c].reshape(nz * length, width).astype(BF16)
        for dy in range(1, ny):
            there = (y + dy) % ny
            part[there, c] = jnp.dot(
                hct_ref[pl.ds(pl.multiple_of(there * rows, 8), rows), :], block, preferred_element_type=F32
            )
            ycopy(c, there).start()
        gw_ref[:, cols(c)] = jnp.dot(
            hct_ref[pl.ds(pl.multiple_of(y * rows, 8), rows), :], block, preferred_element_type=F32
        )
        return carry

    lax.fori_loop(0, chunks, work, 0)

    total = ghp_ref[pl.ds(pl.multiple_of(mine * own_rows, 8), own_rows), :]
    for dt in range(1, ntp):
        harrive(dt).wait_recv()
        total = total + ghland[(mine + dt) % ntp]
    gh_ref[...] = total.astype(gh_ref.dtype)

    def collect(c, carry):
        for dy in range(1, ny):
            there = (y + dy) % ny
            yarrive(c, there).wait_recv()
            gw_ref[:, cols(c)] += land[there, c]
        return carry

    lax.fori_loop(0, chunks, collect, 0)

    def drain(c, carry):
        for dy in range(1, ny):
            ycopy(c, (y + dy) % ny).wait_send()
        for b in range(nz):
            @pl.when((b <= z) & (z < nz - 1))
            def _():
                up(b, c).wait_send()

            @pl.when((b >= z) & (z > 0))
            def _():
                down(b, c).wait_send()

        return carry

    lax.fori_loop(0, chunks, drain, 0)
    for dt in range(1, ntp):
        hcopy(dt).wait_send()


VM = pl.BlockSpec(memory_space=pltpu.VMEM)
LIMIT = 48 * 1024 * 1024


def split(x):
    hi = lax.reduce_precision(x, 8, 7)
    return hi.astype(BF16), (x - hi).astype(BF16)


def two_pass(spec, x, y):
    hi, lo = split(x)
    return jnp.einsum(spec, hi, y, preferred_element_type=F32) + jnp.einsum(spec, lo, y, preferred_element_type=F32)


def per_device(sp, tp, hidden, value_weight, key_vecs, queries, decay_pre, decay_rate, cotangent):
    length = hidden.shape[0]
    heads = decay_rate.shape[0]
    head_width = cotangent.shape[2]
    groups = key_vecs.shape[1]
    state = key_vecs.shape[2]
    per = heads // groups
    features = hidden.shape[1]
    columns = value_weight.shape[1]
    ny = inner_size(sp)
    nz = sp // ny
    values = jnp.dot(hidden, value_weight, preferred_element_type=F32).astype(BF16)
    v = values.reshape(length, groups, per, head_width)
    cot = cotangent.reshape(length, groups, per, head_width)
    log_decay = -decay_rate[None, :] * jax.nn.softplus(decay_pre)
    tri = jnp.tril(jnp.ones((length, length), F32))
    cum = jnp.dot(tri, log_decay, precision=lax.Precision.HIGHEST)
    tot = cum[-1]
    to_end = jnp.exp(tot[None] - cum).reshape(length, groups, per, 1)
    ecum = jnp.exp(cum).reshape(length, groups, per, 1)
    local_state = two_pass("sgip,sgn->gipn", to_end * v.astype(F32), key_vecs)
    local_pull = two_pass("sgip,sgn->gipn", ecum * cot.astype(F32), queries)
    both = jnp.stack([local_state, local_pull], axis=2).reshape(heads, 2, head_width, state)
    dec = jnp.broadcast_to(jnp.exp(tot)[:, None, None], (heads, 1, state))
    span = features // nz
    pieces = 4
    scanned, hcol = pl.pallas_call(
        functools.partial(scan_kernel, ny, nz, tp, 4, pieces),
        out_shape=(
            jax.ShapeDtypeStruct(both.shape, F32),
            jax.ShapeDtypeStruct((nz * length, span), BF16),
        ),
        in_specs=[VM] * 3,
        out_specs=(VM, VM),
        scratch_shapes=[
            pltpu.VMEM((ny,) + both.shape, F32),
            pltpu.VMEM((ny,) + dec.shape, F32),
            pltpu.VMEM((2, heads, head_width, state), F32),
            pltpu.VMEM((2, heads, head_width, state), F32),
            pltpu.VMEM((length, features), F32),
            pltpu.VMEM((nz, length, span), F32),
            pltpu.SemaphoreType.DMA((ny, heads)),
            pltpu.SemaphoreType.DMA((ny, heads)),
            pltpu.SemaphoreType.DMA((ny,)),
            pltpu.SemaphoreType.DMA((ny,)),
            pltpu.SemaphoreType.DMA((2, heads)),
            pltpu.SemaphoreType.DMA((2, heads)),
            pltpu.SemaphoreType.DMA((nz, pieces)),
            pltpu.SemaphoreType.DMA((nz, pieces)),
            pltpu.SemaphoreType.DMA((nz,)),
            pltpu.SemaphoreType.DMA((nz,)),
        ],
        compiler_params=pltpu.CompilerParams(collective_id=0, has_side_effects=True, vmem_limit_bytes=LIMIT),
        name="scan_states",
    )(both, dec, hidden)
    state_in = scanned[:, 0].reshape(groups, per, head_width, state)
    state_grad = scanned[:, 1].reshape(groups, per, head_width, state)

    cum_h = cum.T
    causal = jnp.tril(jnp.ones((length, length), dtype=bool))[None]
    across = cum_h[:, :, None] - cum_h[:, None, :]
    damping = jnp.where(causal, jnp.exp(jnp.where(causal, across, 0.0)), 0.0).reshape(groups, per, length, length)
    scores = jnp.einsum("tgn,sgn->gts", queries, key_vecs, preferred_element_type=F32)
    pair = jnp.einsum("tgip,sgip->gits", cot, v, preferred_element_type=F32)
    dscore = pair * damping
    flux = dscore * scores[:, None]
    net = (jnp.sum(flux, axis=3) - jnp.sum(flux, axis=2)).reshape(heads, length).T
    dsum = jnp.sum(dscore, axis=1)
    mixed = scores[:, None] * damping
    gq_heads = ecum * two_pass("gipn,tgip->tgin", state_in, cot)
    gk_heads = to_end * two_pass("gipn,tgip->tgin", state_grad, v)
    gv = two_pass("gits,tgip->sgip", mixed, cot) + to_end * two_pass(
        "gipn,sgn->sgip", state_grad, key_vecs
    )
    gq = two_pass("gts,sgn->tgn", dsum, key_vecs) + jnp.sum(gq_heads, axis=2)
    gk = two_pass("gts,tgn->sgn", dsum, queries) + jnp.sum(gk_heads, axis=2)
    qgq = jnp.sum(gq_heads * queries.astype(F32)[:, :, None], axis=3).reshape(length, heads)
    kgk = jnp.sum(gk_heads * key_vecs.astype(F32)[:, :, None], axis=3).reshape(length, heads)
    through = jnp.exp(tot) * jnp.sum(state_in * state_grad, axis=(2, 3)).reshape(heads)
    suffix = jnp.dot(tri.T, net + qgq, precision=lax.Precision.HIGHEST)
    prefix = jnp.dot(tri - jnp.eye(length, dtype=F32), kgk, precision=lax.Precision.HIGHEST)
    grad_decay = (suffix + prefix + through[None]) * -decay_rate[None] * jax.nn.sigmoid(decay_pre)

    grad_flat = gv.reshape(length, columns).astype(BF16)
    ghp = lax.dot_general(grad_flat, value_weight, (((1,), (1,)), ((), ())), preferred_element_type=F32)
    rows = features // sp
    width = min(columns, 128)
    chunks = columns // width
    grad_weight, grad_hidden = pl.pallas_call(
        functools.partial(grads_kernel, ny, nz, tp, width),
        out_shape=(
            jax.ShapeDtypeStruct((rows, columns), F32),
            jax.ShapeDtypeStruct((length // tp, features), BF16),
        ),
        in_specs=[VM] * 3,
        out_specs=(VM, VM),
        scratch_shapes=[
            pltpu.VMEM((nz, chunks, length, width), F32),
            pltpu.VMEM((ny, chunks, rows, width), F32),
            pltpu.VMEM((ny, chunks, rows, width), F32),
            pltpu.VMEM((tp, length // tp, features), F32),
            pltpu.SemaphoreType.DMA((nz, chunks)),
            pltpu.SemaphoreType.DMA((nz, chunks)),
            pltpu.SemaphoreType.DMA((nz, chunks)),
            pltpu.SemaphoreType.DMA((ny, chunks)),
            pltpu.SemaphoreType.DMA((ny, chunks)),
            pltpu.SemaphoreType.DMA((tp,)),
            pltpu.SemaphoreType.DMA((tp,)),
        ],
        compiler_params=pltpu.CompilerParams(collective_id=1, has_side_effects=True, vmem_limit_bytes=LIMIT),
        name="weight_grads",
    )(grad_flat.astype(F32), hcol.T, ghp)
    return (gq_cast(gk), gq_cast(gq), grad_decay, grad_hidden, grad_weight)


def gq_cast(x):
    return x.astype(BF16)


def solution(mesh):
    return jax.shard_map(
        functools.partial(per_device, mesh.shape["sp"], mesh.shape["tp"]),
        mesh=mesh,
        in_specs=(
            P("sp", None),
            P(None, "tp"),
            P("sp", "tp", None),
            P("sp", "tp", None),
            P("sp", "tp"),
            P("tp"),
            P("sp", "tp", None),
        ),
        out_specs=(
            P("sp", "tp", None),
            P("sp", "tp", None),
            P("sp", "tp"),
            P(("sp", "tp"), None),
            P("sp", "tp"),
        ),
        check_vma=False,
    )
```
